32 devices in a mesh: grp: 2 (over y), ra: 4 (over z), cb: 4 (over x, core).
Axes of the slice: x: 2, y: 2, z: 4, core: 2. Of those that a mesh axis runs over, the one named last changes fastest.
Arguments:
- tokens: bfloat16 [256, 4096], P('grp', 'ra'), parts along dimension 0, may hold values from -20 to 20
- norm_gain: float32 [4096], P('ra'), may hold values from 0.1 to 1.9
- gate_weight: float32 [4096, 11264], P('ra', 'cb'), may hold values from -0.09375 to 0.09375
- gate_scale: float32 [11264], P('cb'), may hold values from 0.5 to 2
- up_weight: float32 [4096, 11264], P('ra', 'cb'), may hold values from -0.09375 to 0.09375
- up_scale: float32 [11264], P('cb'), may hold values from 0.5 to 2
- down_weight: float32 [11264, 4096], P('cb', 'ra'), may hold values from -1 to 1
- down_scale: float32 [4096], P('ra'), may hold values from 0.5 to 2
- out_gain: float32 [4096], P('ra'), may hold values from 0.1 to 1.9
Outputs:
- normed: bfloat16 [256, 4096], P('grp', 'ra'), parts along dimension 0
The draws below stay inside these ranges and needn't reach their ends.
There are 2 independent parts, one for each index of `grp`. The reference program is written for one: setup_inputs(seed, part) draws one part's arguments, and reference() takes and returns one part's arrays. A program takes and returns all parts, laid end to end along the dimension named above; an argument that names none is the same for every part. Nothing has to cross between parts.
All inputs are finite; a program needn't handle non-finite values.
Results may differ from the reference program's by a relative error of at most 0.012.
Values may be sent and summed in bfloat16 or wider, within the bound.
A program may use at most 64 MiB of HBM per device.

```python
import math
import jax
import jax.numpy as jnp
from jax import lax

D = 4096
FF = 11264
TOK = 128


def draw_tokens(key, part):
    first, second, third = jax.random.split(key, 3)
    base = jnp.clip(jax.random.normal(first, (TOK, D), jnp.float32), -5.0, 5.0)
    place = jnp.arange(D, dtype=jnp.float32) / D
    rows = jnp.exp(jax.random.uniform(second, (TOK, 1), jnp.float32, jnp.log(0.3), jnp.log(3.0)))
    cols = 10.0 ** (place - 1.0) * jax.random.uniform(third, (D,), jnp.float32, 0.7, 1.3)
    values = base * rows * cols
    return values.astype(jnp.bfloat16)


def draw_down_weight(key, part):
    row_key = jax.random.fold_in(key, 101)
    left_key = jax.random.fold_in(key, 102)
    right_key = jax.random.fold_in(key, 103)
    noise_key = jax.random.fold_in(key, 104)
    row_scale = jnp.exp(jax.random.uniform(row_key, (FF, 1), jnp.float32, -1.0, 1.0))
    left = jnp.clip(jax.random.normal(left_key, (FF, 1), jnp.float32), -3.0, 3.0)
    right = jnp.clip(jax.random.normal(right_key, (1, D), jnp.float32), -3.0, 3.0)
    noise = jnp.clip(jax.random.normal(noise_key, (FF, D), jnp.float32), -4.0, 4.0)
    values = row_scale * (0.7 * noise + 0.7 * left * right) * FF ** (-0.5) / 1.35
    return values.astype(jnp.float32)


def block_levels(key, dims, shards, least, largest):
    gain = 1.0
    for axis_at, blocks in shards:
        steps = jax.random.uniform(jax.random.fold_in(jax.random.fold_in(key, 6), axis_at), (blocks,), jnp.float32, least / len(shards), largest / len(shards))
        gain = gain * jnp.repeat(jnp.exp(steps), dims[axis_at] // blocks).reshape((-1,) + (1,) * (len(dims) - 1 - axis_at))
    return gain


def normal_values(key, dims, scale, most, pieces=(), held_as=jnp.bfloat16):
    entries = jax.random.normal(key, dims, jnp.float32) * scale
    if len(pieces) > 0:
        entries = block_levels(key, dims, pieces, -0.22, 0.18) * entries
    return jnp.clip(entries, min=-most, max=most).astype(held_as)


def setup_inputs(seed: int = 0, part: int = 0) -> dict:
    arg_keys = jax.random.split(jax.random.key(seed), 10)
    own_keys = jax.random.split(jax.random.fold_in(arg_keys[9], part), 10)
    return {
        "tokens": draw_tokens(jax.random.fold_in(jax.random.fold_in(arg_keys[9], part), 71), part),
        "norm_gain": jnp.clip(1.0 + 0.18 * jax.random.normal(arg_keys[1], (D,), jnp.float32), 0.1, 1.9),
        "gate_weight": normal_values(arg_keys[2], (D, FF), D ** -0.5, 0.09375, ((0, 4), (1, 4)), jnp.float32),
        "gate_scale": jnp.clip(jnp.exp(math.log(2.0) - 1.3862944 * jax.random.uniform(arg_keys[3], (FF,), jnp.float32) ** block_levels(arg_keys[3], (FF,), ((0, 4),), -0.2, 0.2)), 0.5, 2.0),
        "up_weight": normal_values(arg_keys[4], (D, FF), D ** -0.5, 0.09375, ((0, 4), (1, 4)), jnp.float32),
        "up_scale": jnp.clip(jnp.exp(math.log(2.0) - 1.3862944 * jax.random.uniform(arg_keys[5], (FF,), jnp.float32) ** block_levels(arg_keys[5], (FF,), ((0, 4),), -0.2, 0.2)), 0.5, 2.0),
        "down_weight": draw_down_weight(jax.random.fold_in(arg_keys[9], 71), part),
        "down_scale": jnp.clip(jnp.exp(math.log(2.0) - 1.3862944 * jax.random.uniform(arg_keys[7], (D,), jnp.float32) ** block_levels(arg_keys[7], (D,), ((0, 4),), -0.2, 0.2)), 0.5, 2.0),
        "out_gain": jnp.clip(1.0 + 0.18 * jax.random.normal(arg_keys[8], (D,), jnp.float32), 0.1, 1.9),
    }


def reference(tokens, norm_gain, gate_weight, gate_scale, up_weight, up_scale, down_weight, down_scale, out_gain):
    values = tokens.astype(jnp.float32)
    inv_first = lax.rsqrt(lax.optimization_barrier(jnp.mean(values * values, axis=1, keepdims=True)) + 1e-06)
    normed_in = (values * inv_first * norm_gain).astype(jnp.bfloat16)
    gate = jnp.dot(normed_in, gate_weight.astype(jnp.bfloat16), preferred_element_type=jnp.float32) * gate_scale
    up = jnp.dot(normed_in, up_weight.astype(jnp.bfloat16), preferred_element_type=jnp.float32) * up_scale
    hidden = (jax.nn.silu(gate) * up).astype(jnp.bfloat16)
    branch = jnp.dot(hidden, down_weight.astype(jnp.bfloat16), preferred_element_type=jnp.float32) * down_scale
    mixed = 0.5 * values + branch
    inv_second = lax.rsqrt(lax.optimization_barrier(jnp.mean(mixed * mixed, axis=1, keepdims=True)) + 1e-06)
    return (mixed * inv_second * out_gain).astype(jnp.bfloat16)
```

```python
import functools

import jax
import jax.numpy as jnp
from jax import lax
from jax.experimental import pallas as pl
from jax.experimental.pallas import tpu as pltpu
from jax.sharding import PartitionSpec as P

MESH = pl.DeviceIdType.MESH
F32 = jnp.float32
BF16 = jnp.bfloat16


def plain(tokens, norm_gain, gate_weight, gate_scale, up_weight, up_scale, down_weight, down_scale, out_gain):
    width = tokens.shape[1] * lax.axis_size("ra")
    values = tokens.astype(F32)
    squares = lax.psum(jnp.sum(values * values, axis=1), "ra")
    inv_first = lax.rsqrt(squares / width + 1e-06)[:, None]
    normed_in = (values * inv_first * norm_gain).astype(BF16)
    gate_part = jnp.dot(normed_in, gate_weight.astype(BF16), preferred_element_type=F32)
    up_part = jnp.dot(normed_in, up_weight.astype(BF16), preferred_element_type=F32)
    gate = lax.psum_scatter(gate_part, "ra", scatter_dimension=1, tiled=True)
    up = lax.psum_scatter(up_part, "ra", scatter_dimension=1, tiled=True)
    share = gate.shape[1]
    offset = lax.axis_index("ra") * share
    gate_cols = lax.dynamic_slice_in_dim(gate_scale, offset, share, 0)
    up_cols = lax.dynamic_slice_in_dim(up_scale, offset, share, 0)
    hidden_share = (jax.nn.silu(gate * gate_cols) * (up * up_cols)).astype(BF16)
    partial_value = jnp.dot(
        lax.all_gather(hidden_share, "ra", axis=1, tiled=True),
        down_weight.astype(BF16),
        preferred_element_type=F32,
    )
    branch = lax.psum(partial_value, "cb") * down_scale
    mixed = 0.5 * values + branch
    second = lax.psum(jnp.sum(mixed * mixed, axis=1), "ra")
    inv_second = lax.rsqrt(second / width + 1e-06)[:, None]
    return (mixed * inv_second * out_gain).astype(BF16)


def diagonal(rows, lanes):
    return lax.broadcasted_iota(jnp.int32, (rows, lanes), 0) == lax.broadcasted_iota(jnp.int32, (rows, lanes), 1)


def to_row(col, lanes):
    rows = col.shape[0]
    spread = jnp.where(diagonal(rows, lanes), jnp.broadcast_to(col, (rows, lanes)), 0.0)
    return jnp.broadcast_to(jnp.sum(spread, axis=0, keepdims=True), (8, lanes))


def to_col(row, rows):
    lanes = row.shape[1]
    spread = jnp.where(diagonal(rows, lanes), jnp.broadcast_to(row, (rows, lanes)), 0.0)
    return jnp.sum(spread, axis=1, keepdims=True)


def kernel(
    n, chunks, fc, lag, depth,
    tok_ref, gain_ref, gw_ref, gs_ref, uw_ref, us_ref, dw_ref, ds_ref, og_ref,
    out_ref,
    gw, uw, dw, xg, own, rs_send, rs_recv, hid, acc,
    sq1, sq1_send, inv1, pair_send, pair_recv, x_send, x_recv, sq2, fin,
    w_sem, d_sem, rs_ssem, rs_rsem, ag_ssem, ag_rsem,
    sq1_ssem, sq1_rsem, sq2_ssem, sq2_rsem, misc_s, misc_r,
):
    p = lax.axis_index("ra")
    cb = lax.axis_index("cb")
    core = lax.rem(cb, 2)
    partner = cb + 1 - 2 * core
    x_peer = lax.rem(cb + 2, 4)
    toks, dl = tok_ref.shape
    half = toks // 2
    width = dl * n
    last = n - 1

    def w_copy(c, which):
        src, dst = ((gw_ref, gw), (uw_ref, uw))[which]
        cols = pl.ds(pl.multiple_of(c * fc, fc), fc)
        return pltpu.make_async_copy(src.at[:, cols], dst.at[c], w_sem.at[which, c])

    def d_copy(c):
        rows = pl.ds(pl.multiple_of(c * fc, fc), fc)
        return pltpu.make_async_copy(dw_ref.at[rows, :], dw.at[c], d_sem.at[c])

    for c in range(min(depth, chunks)):
        w_copy(c, 0).start()
        w_copy(c, 1).start()

    barrier = pltpu.get_barrier_semaphore()
    for k in range(1, n):
        pl.semaphore_signal(barrier, inc=1, device_id={"ra": lax.rem(p + k, n)}, device_id_type=MESH)
    for other in (partner, x_peer):
        pl.semaphore_signal(barrier, inc=1, device_id={"cb": other}, device_id_type=MESH)

    values = tok_ref[...].astype(F32)
    xg[...] = (values * gain_ref[...]).astype(BF16)
    sq1_send[...] = to_row(jnp.sum(values * values, axis=1, keepdims=True), toks)
    acc[...] = jnp.zeros_like(acc)

    pl.semaphore_wait(barrier, n + 1)

    def sq1_copy(sender, end):
        return pltpu.make_async_remote_copy(
            src_ref=sq1_send, dst_ref=sq1.at[sender],
            send_sem=sq1_ssem.at[0 if end == 0 else 1], recv_sem=sq1_rsem.at[sender],
            device_id={"ra": end}, device_id_type=MESH)

    for end in (0, last):
        @pl.when(p != end)
        def _():
            sq1_copy(p, end).start()

    def owner_of(f):
        return 0 if f == 0 else last

    def toward(f):
        return jnp.maximum(p - 1, 0) if f == 0 else jnp.minimum(p + 1, last)

    def away(f):
        return toward(1 - f)

    def rs_copy(f, c):
        return pltpu.make_async_remote_copy(
            src_ref=rs_send.at[f, c], dst_ref=rs_recv.at[f, c],
            send_sem=rs_ssem.at[f, c], recv_sem=rs_rsem.at[f, c],
            device_id={"ra": toward(f)}, device_id_type=MESH)

    def ag_copy(f, c):
        return pltpu.make_async_remote_copy(
            src_ref=hid.at[f, c], dst_ref=hid.at[f, c],
            send_sem=ag_ssem.at[f, c], recv_sem=ag_rsem.at[f, c],
            device_id={"ra": away(f)}, device_id_type=MESH)

    def down(f, c):
        rows = slice(f * half, (f + 1) * half)
        acc[rows, :] += jnp.dot(hid[f, c], dw[c].astype(BF16), preferred_element_type=F32)

    def step(t, _):
        @pl.when(t < chunks)
        def _():
            w_copy(t, 0).wait()
            w_copy(t, 1).wait()

            @pl.when(t + depth < chunks)
            def _():
                w_copy(t + depth, 0).start()
                w_copy(t + depth, 1).start()

            @pl.when(t == max(min(chunks - depth, last * lag - 1), 0))
            def _():
                def start(c, _):
                    d_copy(c).start()
                    return 0
                lax.fori_loop(0, chunks, start, 0)

            own[t, :, 0:fc] = jnp.dot(xg[...], gw[t].astype(BF16), preferred_element_type=F32)
            own[t, :, fc:2 * fc] = jnp.dot(xg[...], uw[t].astype(BF16), preferred_element_type=F32)

        @pl.when((t == last * lag) & ((p == 0) | (p == last)))
        def _():
            for k in range(1, n):
                sq1_copy(lax.rem(p + k, n), 0).wait_recv()
            total = jnp.zeros((1, toks), F32)
            for k in range(n):
                total += jnp.where(p == k, sq1_send[0:1, :], sq1[k, 0:1, :])
            inv1[...] = jnp.broadcast_to(lax.rsqrt(to_col(total, toks) / width + 1e-06), inv1.shape)

        for f in (0, 1):
            rank = last - p if f == 0 else p
            c = t - rank * lag
            rows = slice(f * half, (f + 1) * half)
            live = (c >= 0) & (c < chunks)

            @pl.when(live & (rank == 0))
            def _():
                rs_send[f, c] = own[c, rows, :].astype(BF16)
                rs_copy(f, c).start()

            @pl.when(live & (rank > 0))
            def _():
                rs_copy(f, c).wait_recv()

            @pl.when(live & (rank > 0) & (rank < last))
            def _():
                rs_send[f, c] = (own[c, rows, :] + rs_recv[f, c].astype(F32)).astype(BF16)
                rs_copy(f, c).start()

            @pl.when(live & (rank == last))
            def _():
                cols = pl.ds(pl.multiple_of(c * fc, fc), fc)
                scale = inv1[rows, 0:1]
                gate = (own[c, rows, 0:fc] + rs_recv[f, c, :, 0:fc].astype(F32)) * scale * gs_ref[:, cols]
                up = (own[c, rows, fc:2 * fc] + rs_recv[f, c, :, fc:2 * fc].astype(F32)) * scale * us_ref[:, cols]
                hid[f, c] = (gate / (1.0 + jnp.exp(-gate)) * up).astype(BF16)
                ag_copy(f, c).start()

        for f in (0, 1):
            rank = p if f == 0 else last - p
            c = t - (last + rank) * lag
            live = (c >= 0) & (c < chunks)

            @pl.when(live & (rank > 0))
            def _():
                ag_copy(f, c).wait_recv()

            @pl.when(live & (rank > 0) & (rank < last))
            def _():
                ag_copy(f, c).start()

            @pl.when(live)
            def _():
                if f == 0:
                    first = rank <= last - rank
                else:
                    first = rank < last - rank

                @pl.when(first)
                def _():
                    d_copy(c).wait()
                down(f, c)

        return 0

    lax.fori_loop(0, chunks + 2 * last * lag, step, 0)

    def misc_copy(src, dst, k, where):
        return pltpu.make_async_remote_copy(
            src_ref=src, dst_ref=dst, send_sem=misc_s.at[k], recv_sem=misc_r.at[k],
            device_id={"cb": where}, device_id_type=MESH)

    mine = pl.ds(pl.multiple_of(core * half, half), half)
    theirs = pl.ds(pl.multiple_of((1 - core) * half, half), half)
    pair_send[...] = acc[theirs, :].astype(BF16)
    to_pair = misc_copy(pair_send, pair_recv, 0, partner)
    to_pair.start()
    to_pair.wait_recv()
    x_send[...] = (acc[mine, :] + pair_recv[...].astype(F32)).astype(BF16)
    to_x = misc_copy(x_send, x_recv, 1, x_peer)
    to_x.start()
    to_x.wait_recv()
    branch = (x_send[...].astype(F32) + x_recv[...].astype(F32)) * ds_ref[...]
    mixed = 0.5 * tok_ref[mine, :].astype(F32) + branch
    acc[mine, :] = mixed
    sq2[n] = to_row(jnp.sum(mixed * mixed, axis=1, keepdims=True), 128)

    def sq2_copy(sender, k):
        return pltpu.make_async_remote_copy(
            src_ref=sq2.at[n], dst_ref=sq2.at[sender],
            send_sem=sq2_ssem.at[k], recv_sem=sq2_rsem.at[sender],
            device_id={"ra": lax.rem(p + k, n)}, device_id_type=MESH)

    for k in range(1, n):
        sq2_copy(p, k).start()
    for k in range(1, n):
        sq2_copy(lax.rem(p + k, n), k).wait_recv()
    total = jnp.zeros((1, 128), F32)
    for k in range(n):
        total += jnp.where(p == k, sq2[n, 0:1, :], sq2[k, 0:1, :])
    inv2 = lax.rsqrt(to_col(total, half) / width + 1e-06)
    fin[0] = (acc[mine, :] * inv2 * og_ref[...]).astype(BF16)
    to_fin = misc_copy(fin.at[0], fin.at[1], 2, partner)
    to_fin.start()
    out_ref[mine, :] = fin[0]
    to_fin.wait_recv()
    out_ref[theirs, :] = fin[1]

    to_pair.wait_send()
    to_x.wait_send()
    to_fin.wait_send()
    for k in range(1, n):
        sq2_copy(p, k).wait_send()
    for end in (0, last):
        @pl.when(p != end)
        def _():
            sq1_copy(p, end).wait_send()
    for f in (0, 1):
        def drain(c, _):
            @pl.when(p != owner_of(f))
            def _():
                rs_copy(f, c).wait_send()

            @pl.when(p != owner_of(1 - f))
            def _():
                ag_copy(f, c).wait_send()
            return 0
        lax.fori_loop(0, chunks, drain, 0)


FC = 256
LAG = 2
DEPTH = 4


def on_device(tokens, norm_gain, gate_weight, gate_scale, up_weight, up_scale, down_weight, down_scale, out_gain):
    n = lax.axis_size("ra")
    toks, dl = tokens.shape
    ff = gate_weight.shape[1]
    half = toks // 2
    need = 12 * dl * ff + 40 * toks * ff
    if n < 2 or lax.axis_size("cb") != 4 or ff % FC or dl % 128 or toks != 128 or need > 56 * 2**20:
        return plain(tokens, norm_gain, gate_weight, gate_scale, up_weight, up_scale, down_weight, down_scale, out_gain)
    chunks = ff // FC
    vmem = pl.BlockSpec(memory_space=pltpu.VMEM)
    hbm = pl.BlockSpec(memory_space=pl.ANY)
    dma = pltpu.SemaphoreType.DMA
    return pl.pallas_call(
        functools.partial(kernel, n, chunks, FC, LAG, DEPTH),
        out_shape=jax.ShapeDtypeStruct((toks, dl), BF16),
        in_specs=[vmem, vmem, hbm, vmem, hbm, vmem, hbm, vmem, vmem],
        out_specs=vmem,
        scratch_shapes=[
            pltpu.VMEM((chunks, dl, FC), F32),
            pltpu.VMEM((chunks, dl, FC), F32),
            pltpu.VMEM((chunks, FC, dl), F32),
            pltpu.VMEM((toks, dl), BF16),
            pltpu.VMEM((chunks, toks, 2 * FC), F32),
            pltpu.VMEM((2, chunks, half, 2 * FC), BF16),
            pltpu.VMEM((2, chunks, half, 2 * FC), BF16),
            pltpu.VMEM((2, chunks, half, FC), BF16),
            pltpu.VMEM((toks, dl), F32),
            pltpu.VMEM((n, 8, toks), F32),
            pltpu.VMEM((8, toks), F32),
            pltpu.VMEM((toks, 128), F32),
            pltpu.VMEM((half, dl), BF16),
            pltpu.VMEM((half, dl), BF16),
            pltpu.VMEM((half, dl), BF16),
            pltpu.VMEM((half, dl), BF16),
            pltpu.VMEM((n + 1, 8, 128), F32),
            pltpu.VMEM((2, half, dl), BF16),
            dma((2, chunks)),
            dma((chunks,)),
            dma((2, chunks)),
            dma((2, chunks)),
            dma((2, chunks)),
            dma((2, chunks)),
            dma((2,)),
            dma((n,)),
            dma((n,)),
            dma((n,)),
            dma((3,)),
            dma((3,)),
        ],
        compiler_params=pltpu.CompilerParams(
            collective_id=0, has_side_effects=True, vmem_limit_bytes=62 * 2**20
        ),
    )(
        tokens, norm_gain[None, :], gate_weight, gate_scale[None, :], up_weight, up_scale[None, :],
        down_weight, down_scale[None, :], out_gain[None, :],
    )


def solution(mesh):
    return jax.shard_map(
        on_device,
        mesh=mesh,
        in_specs=(
            P("grp", "ra"),
            P("ra"),
            P("ra", "cb"),
            P("cb"),
            P("ra", "cb"),
            P("cb"),
            P("cb", "ra"),
            P("ra"),
            P("ra"),
        ),
        out_specs=P("grp", "ra"),
        check_vma=False,
    )
```

```python
import functools

import jax
import jax.numpy as jnp
from jax import lax
from jax.experimental import pallas as pl
from jax.experimental.pallas import tpu as pltpu
from jax.sharding import PartitionSpec as P

MESH = pl.DeviceIdType.MESH
F32 = jnp.float32
BF16 = jnp.bfloat16


def plain(tokens, norm_gain, gate_weight, gate_scale, up_weight, up_scale, down_weight, down_scale, out_gain):
    width = tokens.shape[1] * lax.axis_size("ra")
    values = tokens.astype(F32)
    squares = lax.psum(jnp.sum(values * values, axis=1), "ra")
    inv_first = lax.rsqrt(squares / width + 1e-06)[:, None]
    normed_in = (values * inv_first * norm_gain).astype(BF16)
    gate_part = jnp.dot(normed_in, gate_weight.astype(BF16), preferred_element_type=F32)
    up_part = jnp.dot(normed_in, up_weight.astype(BF16), preferred_element_type=F32)
    gate = lax.psum_scatter(gate_part, "ra", scatter_dimension=1, tiled=True)
    up = lax.psum_scatter(up_part, "ra", scatter_dimension=1, tiled=True)
    share = gate.shape[1]
    offset = lax.axis_index("ra") * share
    gate_cols = lax.dynamic_slice_in_dim(gate_scale, offset, share, 0)
    up_cols = lax.dynamic_slice_in_dim(up_scale, offset, share, 0)
    hidden_share = (jax.nn.silu(gate * gate_cols) * (up * up_cols)).astype(BF16)
    partial_value = jnp.dot(
        lax.all_gather(hidden_share, "ra", axis=1, tiled=True),
        down_weight.astype(BF16),
        preferred_element_type=F32,
    )
    branch = lax.psum(partial_value, "cb") * down_scale
    mixed = 0.5 * values + branch
    second = lax.psum(jnp.sum(mixed * mixed, axis=1), "ra")
    inv_second = lax.rsqrt(second / width + 1e-06)[:, None]
    return (mixed * inv_second * out_gain).astype(BF16)


def diagonal(rows, lanes):
    return lax.broadcasted_iota(jnp.int32, (rows, lanes), 0) == lax.broadcasted_iota(jnp.int32, (rows, lanes), 1)


def to_row(col, lanes):
    rows = col.shape[0]
    spread = jnp.where(diagonal(rows, lanes), jnp.broadcast_to(col, (rows, lanes)), 0.0)
    return jnp.broadcast_to(jnp.sum(spread, axis=0, keepdims=True), (8, lanes))


def to_col(row, rows):
    lanes = row.shape[1]
    spread = jnp.where(diagonal(rows, lanes), jnp.broadcast_to(row, (rows, lanes)), 0.0)
    return jnp.sum(spread, axis=1, keepdims=True)


def kernel(
    n, chunks, fc, lag, depth,
    tok_ref, gain_ref, gw_ref, gs_ref, uw_ref, us_ref, dw_ref, ds_ref, og_ref,
    out_ref,
    gw, uw, dw, xg, own, rs_send, rs_recv, hid, acc,
    sq1, sq1_send, inv1, scales, pair_send, pair_recv, x_send, x_recv, sq2, fin,
    w_sem, d_sem, rs_ssem, rs_rsem, ag_ssem, ag_rsem,
    sq1_ssem, sq1_rsem, sq2_ssem, sq2_rsem, misc_s, misc_r, s_sem,
):
    p = lax.axis_index("ra")
    cb = lax.axis_index("cb")
    core = lax.rem(cb, 2)
    partner = cb + 1 - 2 * core
    x_peer = lax.rem(cb + 2, 4)
    toks, dl = tok_ref.shape
    half = toks // 2
    width = dl * n
    last = n - 1

    def w_copy(c, which):
        src, dst = ((gw_ref, gw), (uw_ref, uw))[which]
        cols = pl.ds(pl.multiple_of(c * fc, fc), fc)
        return pltpu.make_async_copy(src.at[:, cols], dst.at[c], w_sem.at[which, c])

    def d_copy(c):
        rows = pl.ds(pl.multiple_of(c * fc, fc), fc)
        return pltpu.make_async_copy(dw_ref.at[rows, :], dw.at[c], d_sem.at[c])

    for c in range(min(depth, chunks)):
        w_copy(c, 0).start()
        w_copy(c, 1).start()

    s_copies = [pltpu.make_async_copy(ref, scales.at[k, 0], s_sem.at[k]) for k, ref in enumerate((gs_ref, us_ref))]
    for copy in s_copies:
        copy.start()

    barrier = pltpu.get_barrier_semaphore()
    for k in range(1, n):
        pl.semaphore_signal(barrier, inc=1, device_id={"ra": lax.rem(p + k, n)}, device_id_type=MESH)
    for other in (partner, x_peer):
        pl.semaphore_signal(barrier, inc=1, device_id={"cb": other}, device_id_type=MESH)

    values = tok_ref[...].astype(F32)
    xg[...] = (values * gain_ref[...]).astype(BF16)
    sq1_send[...] = to_row(jnp.sum(values * values, axis=1, keepdims=True), toks)
    acc[...] = jnp.zeros_like(acc)

    for copy in s_copies:
        copy.wait()
    pl.semaphore_wait(barrier, n + 1)

    def sq1_copy(sender, end):
        return pltpu.make_async_remote_copy(
            src_ref=sq1_send, dst_ref=sq1.at[sender],
            send_sem=sq1_ssem.at[0 if end == 0 else 1], recv_sem=sq1_rsem.at[sender],
            device_id={"ra": end}, device_id_type=MESH)

    for end in (0, last):
        @pl.when(p != end)
        def _():
            sq1_copy(p, end).start()

    def owner_of(f):
        return 0 if f == 0 else last

    def toward(f):
        return jnp.maximum(p - 1, 0) if f == 0 else jnp.minimum(p + 1, last)

    def away(f):
        return toward(1 - f)

    def rs_copy(f, c):
        return pltpu.make_async_remote_copy(
            src_ref=rs_send.at[f, c], dst_ref=rs_recv.at[f, c],
            send_sem=rs_ssem.at[f, c], recv_sem=rs_rsem.at[f, c],
            device_id={"ra": toward(f)}, device_id_type=MESH)

    def ag_copy(f, c):
        return pltpu.make_async_remote_copy(
            src_ref=hid.at[f, c], dst_ref=hid.at[f, c],
            send_sem=ag_ssem.at[f, c], recv_sem=ag_rsem.at[f, c],
            device_id={"ra": away(f)}, device_id_type=MESH)

    def down(f, c):
        rows = slice(f * half, (f + 1) * half)
        acc[rows, :] += jnp.dot(hid[f, c], dw[c].astype(BF16), preferred_element_type=F32)

    def step(t, _):
        @pl.when(t < chunks)
        def _():
            w_copy(t, 0).wait()
            w_copy(t, 1).wait()

            @pl.when(t + depth < chunks)
            def _():
                w_copy(t + depth, 0).start()
                w_copy(t + depth, 1).start()

            @pl.when(t == max(min(chunks - depth, last * lag - 1), 0))
            def _():
                def start(c, _):
                    d_copy(c).start()
                    return 0
                lax.fori_loop(0, chunks, start, 0)

            own[t, :, 0:fc] = jnp.dot(xg[...], gw[t].astype(BF16), preferred_element_type=F32)
            own[t, :, fc:2 * fc] = jnp.dot(xg[...], uw[t].astype(BF16), preferred_element_type=F32)

        @pl.when((t == last * lag) & ((p == 0) | (p == last)))
        def _():
            for k in range(1, n):
                sq1_copy(lax.rem(p + k, n), 0).wait_recv()
            total = jnp.zeros((1, toks), F32)
            for k in range(n):
                total += jnp.where(p == k, sq1_send[0:1, :], sq1[k, 0:1, :])
            inv1[...] = jnp.broadcast_to(lax.rsqrt(to_col(total, toks) / width + 1e-06), inv1.shape)

        for f in (0, 1):
            rank = last - p if f == 0 else p
            c = t - rank * lag
            rows = slice(f * half, (f + 1) * half)
            live = (c >= 0) & (c < chunks)

            @pl.when(live & (rank == 0))
            def _():
                rs_send[f, c] = own[c, rows, :].astype(BF16)
                rs_copy(f, c).start()

            @pl.when(live & (rank > 0))
            def _():
                rs_copy(f, c).wait_recv()

            @pl.when(live & (rank > 0) & (rank < last))
            def _():
                rs_send[f, c] = (own[c, rows, :] + rs_recv[f, c].astype(F32)).astype(BF16)
                rs_copy(f, c).start()

            @pl.when(live & (rank == last))
            def _():
                cols = pl.ds(pl.multiple_of(c * fc, fc), fc)
                scale = inv1[rows, 0:1]
                gate = (own[c, rows, 0:fc] + rs_recv[f, c, :, 0:fc].astype(F32)) * scale * scales[0, :, cols]
                up = (own[c, rows, fc:2 * fc] + rs_recv[f, c, :, fc:2 * fc].astype(F32)) * scale * scales[1, :, cols]
                hid[f, c] = (gate / (1.0 + jnp.exp(-gate)) * up).astype(BF16)
                ag_copy(f, c).start()

        for f in (0, 1):
            rank = p if f == 0 else last - p
            c = t - (last + rank) * lag
            live = (c >= 0) & (c < chunks)

            @pl.when(live & (rank > 0))
            def _():
                ag_copy(f, c).wait_recv()

            @pl.when(live & (rank > 0) & (rank < last))
            def _():
                ag_copy(f, c).start()

            @pl.when(live)
            def _():
                if f == 0:
                    first = rank <= last - rank
                else:
                    first = rank < last - rank

                @pl.when(first)
                def _():
                    d_copy(c).wait()
                down(f, c)

        return 0

    lax.fori_loop(0, chunks + 2 * last * lag, step, 0)

    def misc_copy(src, dst, k, where):
        return pltpu.make_async_remote_copy(
            src_ref=src, dst_ref=dst, send_sem=misc_s.at[k], recv_sem=misc_r.at[k],
            device_id={"cb": where}, device_id_type=MESH)

    mine = pl.ds(pl.multiple_of(core * half, half), half)
    theirs = pl.ds(pl.multiple_of((1 - core) * half, half), half)
    pair_send[...] = acc[theirs, :].astype(BF16)
    to_pair = misc_copy(pair_send, pair_recv, 0, partner)
    to_pair.start()
    to_pair.wait_recv()
    x_send[...] = (acc[mine, :] + pair_recv[...].astype(F32)).astype(BF16)
    to_x = misc_copy(x_send, x_recv, 1, x_peer)
    to_x.start()
    to_x.wait_recv()
    branch = (x_send[...].astype(F32) + x_recv[...].astype(F32)) * ds_ref[...]
    mixed = 0.5 * tok_ref[mine, :].astype(F32) + branch
    acc[mine, :] = mixed
    sq2[n] = to_row(jnp.sum(mixed * mixed, axis=1, keepdims=True), 128)

    def sq2_copy(sender, k):
        return pltpu.make_async_remote_copy(
            src_ref=sq2.at[n], dst_ref=sq2.at[sender],
            send_sem=sq2_ssem.at[k], recv_sem=sq2_rsem.at[sender],
            device_id={"ra": lax.rem(p + k, n)}, device_id_type=MESH)

    for k in range(1, n):
        sq2_copy(p, k).start()
    for k in range(1, n):
        sq2_copy(lax.rem(p + k, n), k).wait_recv()
    total = jnp.zeros((1, 128), F32)
    for k in range(n):
        total += jnp.where(p == k, sq2[n, 0:1, :], sq2[k, 0:1, :])
    inv2 = lax.rsqrt(to_col(total, half) / width + 1e-06)
    fin[0] = (acc[mine, :] * inv2 * og_ref[...]).astype(BF16)
    to_fin = misc_copy(fin.at[0], fin.at[1], 2, partner)
    to_fin.start()
    out_ref[mine, :] = fin[0]
    to_fin.wait_recv()
    out_ref[theirs, :] = fin[1]

    to_pair.wait_send()
    to_x.wait_send()
    to_fin.wait_send()
    for k in range(1, n):
        sq2_copy(p, k).wait_send()
    for end in (0, last):
        @pl.when(p != end)
        def _():
            sq1_copy(p, end).wait_send()
    for f in (0, 1):
        def drain(c, _):
            @pl.when(p != owner_of(f))
            def _():
                rs_copy(f, c).wait_send()

            @pl.when(p != owner_of(1 - f))
            def _():
                ag_copy(f, c).wait_send()
            return 0
        lax.fori_loop(0, chunks, drain, 0)


FC = 256
LAG = 4
DEPTH = 2


def on_device(tokens, norm_gain, gate_weight, gate_scale, up_weight, up_scale, down_weight, down_scale, out_gain):
    n = lax.axis_size("ra")
    toks, dl = tokens.shape
    ff = gate_weight.shape[1]
    half = toks // 2
    need = 12 * dl * ff + 40 * toks * ff
    if n < 2 or lax.axis_size("cb") != 4 or ff % FC or dl % 128 or toks != 128 or need > 56 * 2**20:
        return plain(tokens, norm_gain, gate_weight, gate_scale, up_weight, up_scale, down_weight, down_scale, out_gain)
    chunks = ff // FC
    vmem = pl.BlockSpec(memory_space=pltpu.VMEM)
    hbm = pl.BlockSpec(memory_space=pl.ANY)
    dma = pltpu.SemaphoreType.DMA
    return pl.pallas_call(
        functools.partial(kernel, n, chunks, FC, LAG, DEPTH),
        out_shape=jax.ShapeDtypeStruct((toks, dl), BF16),
        in_specs=[vmem, vmem, hbm, hbm, hbm, hbm, hbm, vmem, vmem],
        out_specs=vmem,
        scratch_shapes=[
            pltpu.VMEM((chunks, dl, FC), F32),
            pltpu.VMEM((chunks, dl, FC), F32),
            pltpu.VMEM((chunks, FC, dl), F32),
            pltpu.VMEM((toks, dl), BF16),
            pltpu.VMEM((chunks, toks, 2 * FC), F32),
            pltpu.VMEM((2, chunks, half, 2 * FC), BF16),
            pltpu.VMEM((2, chunks, half, 2 * FC), BF16),
            pltpu.VMEM((2, chunks, half, FC), BF16),
            pltpu.VMEM((toks, dl), F32),
            pltpu.VMEM((n, 8, toks), F32),
            pltpu.VMEM((8, toks), F32),
            pltpu.VMEM((toks, 128), F32),
            pltpu.VMEM((2, 1, ff), F32),
            pltpu.VMEM((half, dl), BF16),
            pltpu.VMEM((half, dl), BF16),
            pltpu.VMEM((half, dl), BF16),
            pltpu.VMEM((half, dl), BF16),
            pltpu.VMEM((n + 1, 8, 128), F32),
            pltpu.VMEM((2, half, dl), BF16),
            dma((2, chunks)),
            dma((chunks,)),
            dma((2, chunks)),
            dma((2, chunks)),
            dma((2, chunks)),
            dma((2, chunks)),
            dma((2,)),
            dma((n,)),
            dma((n,)),
            dma((n,)),
            dma((3,)),
            dma((3,)),
            dma((2,)),
        ],
        compiler_params=pltpu.CompilerParams(
            collective_id=0, has_side_effects=True, vmem_limit_bytes=62 * 2**20
        ),
    )(
        tokens, norm_gain[None, :], gate_weight, gate_scale, up_weight, up_scale,
        down_weight, down_scale[None, :], out_gain[None, :],
    )


def solution(mesh):
    return jax.shard_map(
        on_device,
        mesh=mesh,
        in_specs=(
            P("grp", "ra"),
            P("ra"),
            P("ra", "cb"),
            P("cb"),
            P("ra", "cb"),
            P("cb"),
            P("cb", "ra"),
            P("ra"),
            P("ra"),
        ),
        out_specs=P("grp", "ra"),
        check_vma=False,
    )
```

```python
import functools

import jax
import jax.numpy as jnp
from jax import lax
from jax.experimental import pallas as pl
from jax.experimental.pallas import tpu as pltpu
from jax.sharding import PartitionSpec as P

MESH = pl.DeviceIdType.MESH
F32 = jnp.float32
BF16 = jnp.bfloat16


def plain(tokens, norm_gain, gate_weight, gate_scale, up_weight, up_scale, down_weight, down_scale, out_gain):
    width = tokens.shape[1] * lax.axis_size("ra")
    values = tokens.astype(F32)
    squares = lax.psum(jnp.sum(values * values, axis=1), "ra")
    inv_first = lax.rsqrt(squares / width + 1e-06)[:, None]
    normed_in = (values * inv_first * norm_gain).astype(BF16)
    gate_part = jnp.dot(normed_in, gate_weight.astype(BF16), preferred_element_type=F32)
    up_part = jnp.dot(normed_in, up_weight.astype(BF16), preferred_element_type=F32)
    gate = lax.psum_scatter(gate_part, "ra", scatter_dimension=1, tiled=True)
    up = lax.psum_scatter(up_part, "ra", scatter_dimension=1, tiled=True)
    share = gate.shape[1]
    offset = lax.axis_index("ra") * share
    gate_cols = lax.dynamic_slice_in_dim(gate_scale, offset, share, 0)
    up_cols = lax.dynamic_slice_in_dim(up_scale, offset, share, 0)
    hidden_share = (jax.nn.silu(gate * gate_cols) * (up * up_cols)).astype(BF16)
    partial_value = jnp.dot(
        lax.all_gather(hidden_share, "ra", axis=1, tiled=True),
        down_weight.astype(BF16),
        preferred_element_type=F32,
    )
    branch = lax.psum(partial_value, "cb") * down_scale
    mixed = 0.5 * values + branch
    second = lax.psum(jnp.sum(mixed * mixed, axis=1), "ra")
    inv_second = lax.rsqrt(second / width + 1e-06)[:, None]
    return (mixed * inv_second * out_gain).astype(BF16)


def diagonal(rows, lanes):
    return lax.broadcasted_iota(jnp.int32, (rows, lanes), 0) == lax.broadcasted_iota(jnp.int32, (rows, lanes), 1)


def to_row(col, lanes):
    rows = col.shape[0]
    spread = jnp.where(diagonal(rows, lanes), jnp.broadcast_to(col, (rows, lanes)), 0.0)
    return jnp.broadcast_to(jnp.sum(spread, axis=0, keepdims=True), (8, lanes))


def to_col(row, rows):
    lanes = row.shape[1]
    spread = jnp.where(diagonal(rows, lanes), jnp.broadcast_to(row, (rows, lanes)), 0.0)
    return jnp.sum(spread, axis=1, keepdims=True)


def kernel(
    n, chunks, fc, lag, depth,
    tok_hbm, gain_hbm, gw_ref, gs_ref, uw_ref, us_ref, dw_ref, ds_hbm, og_hbm,
    out_ref, tok_ref, gain_ref, ds_ref, og_ref,
    gw, uw, dw, xg, own, rs_send, rs_recv, hid, acc,
    sq1, sq1_send, inv1, scales, pair_send, pair_recv, x_send, x_recv, sq2, mixed, fin,
    w_sem, d_sem, rs_ssem, rs_rsem, ag_ssem, ag_rsem,
    sq1_ssem, sq1_rsem, sq2_ssem, sq2_rsem, misc_s, misc_r, s_sem, i_sem,
):
    p = lax.axis_index("ra")
    cb = lax.axis_index("cb")
    core = lax.rem(cb, 2)
    partner = cb + 1 - 2 * core
    x_peer = lax.rem(cb + 2, 4)
    toks, dl = tok_hbm.shape
    half = toks // 2
    width = dl * n
    last = n - 1

    def w_copy(c, which):
        src, dst = ((gw_ref, gw), (uw_ref, uw))[which]
        cols = pl.ds(pl.multiple_of(c * fc, fc), fc)
        return pltpu.make_async_copy(src.at[:, cols], dst.at[c], w_sem.at[which, c])

    def d_copy(c):
        rows = pl.ds(pl.multiple_of(c * fc, fc), fc)
        return pltpu.make_async_copy(dw_ref.at[rows, :], dw.at[c], d_sem.at[c])

    pairs = ((tok_hbm, tok_ref), (gain_hbm, gain_ref), (ds_hbm, ds_ref), (og_hbm, og_ref))
    i_copies = [pltpu.make_async_copy(a, b, i_sem.at[k]) for k, (a, b) in enumerate(pairs)]
    for copy in i_copies:
        copy.start()
    for c in range(min(depth, chunks)):
        w_copy(c, 0).start()
        w_copy(c, 1).start()

    s_copies = [pltpu.make_async_copy(ref, scales.at[k, 0], s_sem.at[k]) for k, ref in enumerate((gs_ref, us_ref))]
    for copy in s_copies:
        copy.start()

    barrier = pltpu.get_barrier_semaphore()
    for k in range(1, n):
        pl.semaphore_signal(barrier, inc=1, device_id={"ra": lax.rem(p + k, n)}, device_id_type=MESH)
    for other in (partner, x_peer):
        pl.semaphore_signal(barrier, inc=1, device_id={"cb": other}, device_id_type=MESH)

    for copy in i_copies:
        copy.wait()
    values = tok_ref[...].astype(F32)
    xg[...] = (values * gain_ref[...]).astype(BF16)
    sq1_send[...] = to_row(jnp.sum(values * values, axis=1, keepdims=True), toks)
    acc[...] = jnp.zeros_like(acc)

    for copy in s_copies:
        copy.wait()
    pl.semaphore_wait(barrier, n + 1)

    def sq1_copy(sender, end):
        return pltpu.make_async_remote_copy(
            src_ref=sq1_send, dst_ref=sq1.at[sender],
            send_sem=sq1_ssem.at[0 if end == 0 else 1], recv_sem=sq1_rsem.at[sender],
            device_id={"ra": end}, device_id_type=MESH)

    for end in (0, last):
        @pl.when(p != end)
        def _():
            sq1_copy(p, end).start()

    def owner_of(f):
        return 0 if f == 0 else last

    def toward(f):
        return jnp.maximum(p - 1, 0) if f == 0 else jnp.minimum(p + 1, last)

    def away(f):
        return toward(1 - f)

    def rs_copy(f, c):
        return pltpu.make_async_remote_copy(
            src_ref=rs_send.at[f, c], dst_ref=rs_recv.at[f, c],
            send_sem=rs_ssem.at[f, c], recv_sem=rs_rsem.at[f, c],
            device_id={"ra": toward(f)}, device_id_type=MESH)

    def ag_copy(f, c):
        return pltpu.make_async_remote_copy(
            src_ref=hid.at[f, c], dst_ref=hid.at[f, c],
            send_sem=ag_ssem.at[f, c], recv_sem=ag_rsem.at[f, c],
            device_id={"ra": away(f)}, device_id_type=MESH)

    def down(f, c):
        rows = slice(f * half, (f + 1) * half)
        acc[rows, :] += jnp.dot(hid[f, c], dw[c].astype(BF16), preferred_element_type=F32)

    def step(t, _):
        @pl.when(t < chunks)
        def _():
            w_copy(t, 0).wait()
            w_copy(t, 1).wait()

            @pl.when(t + depth < chunks)
            def _():
                w_copy(t + depth, 0).start()
                w_copy(t + depth, 1).start()

            @pl.when(t == max(min(chunks - depth, last * lag - 1), 0))
            def _():
                def start(c, _):
                    d_copy(c).start()
                    return 0
                lax.fori_loop(0, chunks, start, 0)

            own[t, :, 0:fc] = jnp.dot(xg[...], gw[t].astype(BF16), preferred_element_type=F32)
            own[t, :, fc:2 * fc] = jnp.dot(xg[...], uw[t].astype(BF16), preferred_element_type=F32)

        @pl.when((t == last * lag) & ((p == 0) | (p == last)))
        def _():
            for k in range(1, n):
                sq1_copy(lax.rem(p + k, n), 0).wait_recv()
            total = jnp.zeros((1, toks), F32)
            for k in range(n):
                total += jnp.where(p == k, sq1_send[0:1, :], sq1[k, 0:1, :])
            inv1[...] = jnp.broadcast_to(lax.rsqrt(to_col(total, toks) / width + 1e-06), inv1.shape)

        for f in (0, 1):
            rank = last - p if f == 0 else p
            c = t - rank * lag
            rows = slice(f * half, (f + 1) * half)
            live = (c >= 0) & (c < chunks)

            @pl.when(live & (rank == 0))
            def _():
                rs_send[f, c] = own[c, rows, :].astype(BF16)
                rs_copy(f, c).start()

            @pl.when(live & (rank > 0))
            def _():
                rs_copy(f, c).wait_recv()

            @pl.when(live & (rank > 0) & (rank < last))
            def _():
                rs_send[f, c] = (own[c, rows, :] + rs_recv[f, c].astype(F32)).astype(BF16)
                rs_copy(f, c).start()

            @pl.when(live & (rank == last))
            def _():
                cols = pl.ds(pl.multiple_of(c * fc, fc), fc)
                scale = inv1[rows, 0:1]
                gate = (own[c, rows, 0:fc] + rs_recv[f, c, :, 0:fc].astype(F32)) * scale * scales[0, :, cols]
                up = (own[c, rows, fc:2 * fc] + rs_recv[f, c, :, fc:2 * fc].astype(F32)) * scale * scales[1, :, cols]
                hid[f, c] = (gate / (1.0 + jnp.exp(-gate)) * up).astype(BF16)
                ag_copy(f, c).start()

        for f in (0, 1):
            rank = p if f == 0 else last - p
            c = t - (last + rank) * lag
            live = (c >= 0) & (c < chunks)

            @pl.when(live & (rank > 0))
            def _():
                ag_copy(f, c).wait_recv()

            @pl.when(live & (rank > 0) & (rank < last))
            def _():
                ag_copy(f, c).start()

        for f in (0, 1):
            rank = p if f == 0 else last - p
            c = t - (last + rank) * lag

            @pl.when((c >= 0) & (c < chunks))
            def _():
                if f == 0:
                    first = rank <= last - rank
                else:
                    first = rank < last - rank

                @pl.when(first)
                def _():
                    d_copy(c).wait()
                down(f, c)

        for f in (0, 1):
            rank = p if f == 0 else last - p
            t0 = chunks + (last + rank) * lag
            kept = slice(f * quarter, (f + 1) * quarter)

            @pl.when(t == t0)
            def _():
                pair_send[f] = acc[rows_of(f, 1 - core), :].astype(BF16)
                pair_copy(f).start()

            @pl.when(t == t0 + 2)
            def _():
                pair_copy(f).wait_recv()
                x_send[f] = (acc[rows_of(f, core), :] + pair_recv[f].astype(F32)).astype(BF16)
                x_copy(f).start()

            @pl.when(t == t0 + 6)
            def _():
                x_copy(f).wait_recv()
                branch = (x_send[f].astype(F32) + x_recv[f].astype(F32)) * ds_ref[...]
                new = 0.5 * tok_ref[rows_of(f, core), :].astype(F32) + branch
                mixed[kept, :] = new
                sq2[f, n] = to_row(jnp.sum(new * new, axis=1, keepdims=True), 128)
                for k in range(1, n):
                    sq2_copy(f, p, k).start()

        return 0

    quarter = half // 2

    def rows_of(f, which):
        return pl.ds(pl.multiple_of(f * half + which * quarter, quarter), quarter)

    def misc_copy(src, dst, k, where):
        return pltpu.make_async_remote_copy(
            src_ref=src, dst_ref=dst, send_sem=misc_s.at[k], recv_sem=misc_r.at[k],
            device_id={"cb": where}, device_id_type=MESH)

    def pair_copy(f):
        return misc_copy(pair_send.at[f], pair_recv.at[f], f, partner)

    def x_copy(f):
        return misc_copy(x_send.at[f], x_recv.at[f], 2 + f, x_peer)

    def sq2_copy(f, sender, k):
        return pltpu.make_async_remote_copy(
            src_ref=sq2.at[f, n], dst_ref=sq2.at[f, sender],
            send_sem=sq2_ssem.at[f, k], recv_sem=sq2_rsem.at[f, sender],
            device_id={"ra": lax.rem(p + k, n)}, device_id_type=MESH)

    lax.fori_loop(0, chunks + 2 * last * lag + 7, step, 0)

    for f in (0, 1):
        for k in range(1, n):
            sq2_copy(f, lax.rem(p + k, n), k).wait_recv()
        total = jnp.zeros((1, 128), F32)
        for k in range(n):
            total += jnp.where(p == k, sq2[f, n, 0:1, :], sq2[f, k, 0:1, :])
        inv2 = lax.rsqrt(to_col(total, quarter) / width + 1e-06)
        kept = slice(f * quarter, (f + 1) * quarter)
        fin[0, kept, :] = (mixed[kept, :] * inv2 * og_ref[...]).astype(BF16)
    to_fin = misc_copy(fin.at[0], fin.at[1], 4, partner)
    to_fin.start()
    for f in (0, 1):
        out_ref[rows_of(f, core), :] = fin[0, f * quarter:(f + 1) * quarter, :]
    to_fin.wait_recv()
    for f in (0, 1):
        out_ref[rows_of(f, 1 - core), :] = fin[1, f * quarter:(f + 1) * quarter, :]

    to_fin.wait_send()
    for f in (0, 1):
        pair_copy(f).wait_send()
        x_copy(f).wait_send()
        for k in range(1, n):
            sq2_copy(f, p, k).wait_send()
    for end in (0, last):
        @pl.when(p != end)
        def _():
            sq1_copy(p, end).wait_send()
    for f in (0, 1):
        def drain(c, _):
            @pl.when(p != owner_of(f))
            def _():
                rs_copy(f, c).wait_send()

            @pl.when(p != owner_of(1 - f))
            def _():
                ag_copy(f, c).wait_send()
            return 0
        lax.fori_loop(0, chunks, drain, 0)


FC = 256
LAG = 3
DEPTH = 2


def on_device(tokens, norm_gain, gate_weight, gate_scale, up_weight, up_scale, down_weight, down_scale, out_gain):
    n = lax.axis_size("ra")
    toks, dl = tokens.shape
    ff = gate_weight.shape[1]
    half = toks // 2
    need = 12 * dl * ff + 40 * toks * ff
    if n < 2 or lax.axis_size("cb") != 4 or ff % FC or dl % 128 or toks != 128 or need > 56 * 2**20:
        return plain(tokens, norm_gain, gate_weight, gate_scale, up_weight, up_scale, down_weight, down_scale, out_gain)
    chunks = ff // FC
    vmem = pl.BlockSpec(memory_space=pltpu.VMEM)
    hbm = pl.BlockSpec(memory_space=pl.ANY)
    dma = pltpu.SemaphoreType.DMA
    return pl.pallas_call(
        functools.partial(kernel, n, chunks, FC, LAG, DEPTH),
        out_shape=jax.ShapeDtypeStruct((toks, dl), BF16),
        in_specs=[hbm] * 9,
        out_specs=vmem,
        scratch_shapes=[
            pltpu.VMEM((toks, dl), BF16),
            pltpu.VMEM((1, dl), F32),
            pltpu.VMEM((1, dl), F32),
            pltpu.VMEM((1, dl), F32),
            pltpu.VMEM((chunks, dl, FC), F32),
            pltpu.VMEM((chunks, dl, FC), F32),
            pltpu.VMEM((chunks, FC, dl), F32),
            pltpu.VMEM((toks, dl), BF16),
            pltpu.VMEM((chunks, toks, 2 * FC), F32),
            pltpu.VMEM((2, chunks, half, 2 * FC), BF16),
            pltpu.VMEM((2, chunks, half, 2 * FC), BF16),
            pltpu.VMEM((2, chunks, half, FC), BF16),
            pltpu.VMEM((toks, dl), F32),
            pltpu.VMEM((n, 8, toks), F32),
            pltpu.VMEM((8, toks), F32),
            pltpu.VMEM((toks, 128), F32),
            pltpu.VMEM((2, 1, ff), F32),
            pltpu.VMEM((2, half // 2, dl), BF16),
            pltpu.VMEM((2, half // 2, dl), BF16),
            pltpu.VMEM((2, half // 2, dl), BF16),
            pltpu.VMEM((2, half // 2, dl), BF16),
            pltpu.VMEM((2, n + 1, 8, 128), F32),
            pltpu.VMEM((half, dl), F32),
            pltpu.VMEM((2, half, dl), BF16),
            dma((2, chunks)),
            dma((chunks,)),
            dma((2, chunks)),
            dma((2, chunks)),
            dma((2, chunks)),
            dma((2, chunks)),
            dma((2,)),
            dma((n,)),
            dma((2, n)),
            dma((2, n)),
            dma((5,)),
            dma((5,)),
            dma((2,)),
            dma((4,)),
        ],
        compiler_params=pltpu.CompilerParams(
            collective_id=0, has_side_effects=True, vmem_limit_bytes=62 * 2**20
        ),
    )(
        tokens, norm_gain[None, :], gate_weight, gate_scale, up_weight, up_scale,
        down_weight, down_scale[None, :], out_gain[None, :],
    )


def solution(mesh):
    return jax.shard_map(
        on_device,
        mesh=mesh,
        in_specs=(
            P("grp", "ra"),
            P("ra"),
            P("ra", "cb"),
            P("cb"),
            P("ra", "cb"),
            P("cb"),
            P("cb", "ra"),
            P("ra"),
            P("ra"),
        ),
        out_specs=P("grp", "ra"),
        check_vma=False,
    )
```
